32 devices in a mesh: sp: 4 (over y, x), tp: 8 (over z, core).
Axes of the slice: x: 2, y: 2, z: 4, core: 2. Of those that a mesh axis runs over, the one named last changes fastest.
Arguments:
- cotangent: bfloat16 [1024, 2048], P('sp', 'tp'), may hold values from -6 to 6
- block_input: bfloat16 [1024, 2048], P('sp', 'tp'), may hold values from -6 to 6
- routes: int32 [1024, 2], P('sp'), may hold values from 0 to 3, all different within a row; in each aligned block of 256 rows (0 to 255, 256 to 511, ...) at most 160 rows name the same one
- route_weights: float32 [1024, 2], P('sp'), may hold values from 0.1 to 0.9
- gate_weight: bfloat16 [4, 2048, 7168], P('sp', None, 'tp'), may hold values from -0.125 to 0.125
- up_weight: bfloat16 [4, 2048, 7168], P('sp', None, 'tp'), may hold values from -0.125 to 0.125
- down_weight: bfloat16 [4, 7168, 2048], P('sp', 'tp'), may hold values from -0.0625 to 0.0625
- out_weight: bfloat16 [1024, 2048], P('tp'), may hold values from -0.1875 to 0.1875
- conv_out: bfloat16 [1024, 1024], P('tp', 'sp'), may hold values from -6 to 6
- gate_pre: bfloat16 [1024, 1024], P('tp', 'sp'), may hold values from -6 to 6
- prior_states: bfloat16 [1024, 1024], P('tp', 'sp'), may hold values from -6 to 6
- recur_weight: bfloat16 [16, 64, 64], replicated, may hold values from -0.75 to 0.75
- input_gate_matrix: bfloat16 [16, 64, 64], replicated, may hold values from -0.75 to 0.75
- decay_param: float32 [1024], replicated, may hold values from 4 to 16
- decay_jump: float32 [1024, 1024], P('tp', 'sp'), may hold values from -1 to 0, as said below
Outputs:
- gate_weight_grad: bfloat16 [4, 2048, 7168], P('sp', None, 'tp')
- up_weight_grad: bfloat16 [4, 2048, 7168], P('sp', None, 'tp')
- down_weight_grad: bfloat16 [4, 7168, 2048], P('sp', 'tp')
- out_weight_grad: float32 [1024, 2048], P('tp', 'sp')
- conv_grad: bfloat16 [1024, 1024], P('tp', 'sp')
- valve_logit_derivative: bfloat16 [1024, 1024], P('tp', 'sp')
The draws below stay inside these ranges and needn't reach their ends.
Inputs may be any that keep to these rules, and one draw needn't show every extreme that they name: In each aligned block of 256 rows (the rows of one index of sp) no expert is named by more than 160 routes, a bound that some block reaches; a row names 2 different experts. `decay_jump`: every entry is at most -1 / 20480.
All inputs are finite; a program needn't handle non-finite values.
Results may differ from the reference program's by a relative error of at most 0.018.
Values may be sent and summed in bfloat16 or wider, within the bound.
A program may use at most 128 MiB of HBM per device.

```python
import math
import jax
import jax.numpy as jnp
import numpy as np
from jax import lax

D = 2048
HEAD_DIM = 64
HEADS = 16
FF = 7168
TOP_K = 2
TOK_DEV = 256
WIDTH = 1024
EXPERTS = 4
TOKENS = 1024
CAP = 160
N_SP = 4
N_TP = 8


def draw_decay_param(key, part):
    keys = jax.random.split(jax.random.fold_in(key, 11), 3)
    share = 0.5
    fast = jax.random.uniform(keys[0], (WIDTH,), jnp.float32) < share
    fast_rate = jnp.exp(jax.random.uniform(keys[1], (WIDTH,), jnp.float32, jnp.log(1.0 / 400.0), jnp.log(1.0 / 100.0)))
    slow_rate = jnp.exp(jax.random.uniform(keys[2], (WIDTH,), jnp.float32, jnp.log(0.1), jnp.log(0.8))) / (8.0 * TOKENS)
    rate = jnp.where(fast, fast_rate, slow_rate)
    return (-jnp.log(jnp.expm1(rate))).astype(jnp.float32)


def draw_decay_jump(key, part):
    keys = jax.random.split(jax.random.fold_in(key, 23), 3)
    blocks = TOKENS // TOK_DEV
    block_rate = jnp.exp(jax.random.uniform(keys[0], (WIDTH, blocks), jnp.float32, jnp.log(0.05), jnp.log(0.4))) / TOKENS
    settled_regime = jnp.repeat(block_rate, TOK_DEV, axis=1)
    deposit_items = jax.random.randint(keys[1], (2,), 0, TOKENS)
    objective_numbers = jnp.log(jax.random.uniform(keys[2], (WIDTH, 2), jnp.float32, 0.6, 0.8))
    sequence_indices = jnp.arange(TOKENS)[None, :]
    clustered_bundles = jnp.where(sequence_indices == deposit_items[0], objective_numbers[:, 0:1], 0.0) + jnp.where(sequence_indices == deposit_items[1], objective_numbers[:, 1:2], 0.0)
    return (clustered_bundles - settled_regime).astype(jnp.float32)


def spiked(array, stream_key, source, target, blocks, factor):
    def block_of(axis_at):
        return (jnp.arange(array.shape[axis_at]) // (array.shape[axis_at] // blocks)).reshape((-1,) + (1,) * (array.ndim - 1 - axis_at))

    first = jax.random.permutation(stream_key, blocks)[block_of(target)]
    far = (block_of(target) + blocks // 2) % blocks
    return jnp.where((block_of(source) == first) | (block_of(source) == far), factor * array, array)


def steps_of(own_key, dims, cuts, smallest, top_value):
    def one(dim, blocks):
        steps = jax.random.uniform(jax.random.fold_in(jax.random.fold_in(own_key, 6), dim), (blocks,), jnp.float32, smallest / len(cuts), top_value / len(cuts))
        return jnp.repeat(jnp.exp(steps), dims[dim] // blocks).reshape((-1,) + (1,) * (len(dims) - dim - 1))

    factor_of = one(*cuts[0])
    for cut in cuts[1:]:
        factor_of = factor_of * one(*cut)
    return factor_of


def routed_block(own_key, own, number, rows, amount, top, limit, lean):
    order = jax.random.permutation(own_key, amount)
    packed, usual = portions_of(amount, rows * top, limit, lean, True), portions_of(amount, rows * top, limit, lean, False)
    places = jnp.arange(amount)

    def named(lengths, turn):
        used = int((lengths > 0).sum())
        fixed = max(1, used // 4)
        passed = fixed + (places - fixed + turn * (used - fixed)) % max(1, amount - fixed)
        return jnp.zeros((amount,), jnp.int32).at[order[jnp.where(places < fixed, places, passed)]].set(jnp.asarray(lengths, jnp.int32))

    lengths = jnp.where(number % 4 == 0, named(packed, number // 4), named(usual, number - number // 4 - 1))
    mixed = jax.random.permutation(jax.random.fold_in(own, 3), amount)
    donor, taker = mixed[0:amount // 2 * 2:2], mixed[1:amount // 2 * 2:2]
    room = jnp.minimum(lengths[donor] - 1, limit - lengths[taker]) // 2
    room = jnp.where((donor == order[0]) | (taker == order[0]) | (lengths[taker] == 0), 0, jnp.maximum(room, 0))
    passed = jax.random.randint(jax.random.fold_in(own, 4), (amount // 2,), 0, 1 << 20) % (room + 1)
    lengths = lengths.at[donor].add(-passed).at[taker].add(passed)
    items = jnp.searchsorted(jnp.cumsum(lengths), jnp.arange(rows * top), side="right").astype(jnp.int32)
    listing = items.reshape(top, rows).T
    listing = listing[jax.random.permutation(jax.random.fold_in(own, 1), rows)]
    turn = jax.random.randint(jax.random.fold_in(own, 2), (rows, 1), 0, top)
    return jnp.take_along_axis(listing, (jnp.arange(top)[None, :] + turn) % top, axis=1)


def portions_of(amount, total, reach, lean, full):
    loads = [(1 << 20) // math.isqrt(standing ** lean) + 1 for standing in range(1, amount + 1)]
    largest = reach if full else min(reach, max(-(-total // amount), total * loads[0] // sum(loads)))
    least = 1 if total - largest >= amount - 1 else 0
    given, rest = [largest] + [least] * (amount - 1), total - largest - least * (amount - 1)
    while rest > 0:
        free = [i for i in range(1, amount) if given[i] < largest] or [i for i in range(1, amount) if given[i] < reach]
        whole, budget = sum([loads[i] for i in free]), rest
        for i in free:
            extra = min(reach - given[i], max(1, budget * loads[i] // whole), rest)
            given[i] = given[i] + extra
            rest = rest - extra
    return np.array(given)


def noise(own_key, shape, deviation, reach, cuts=(), kind=jnp.bfloat16):
    array = deviation * jax.random.normal(own_key, shape, jnp.float32)
    if cuts:
        array = array * steps_of(own_key, shape, cuts, -0.22, 0.18)
    return jnp.clip(array, -reach, reach).astype(kind)


def heavy_noise(own_key, extent, scale, limit, cuts, heavy, kind=jnp.bfloat16):
    values = scale * jax.random.normal(own_key, extent, jnp.float32)
    if cuts:
        values = values * steps_of(own_key, extent, cuts, -0.22, 0.18)
    return jnp.clip(spiked(values, jax.random.fold_in(own_key, 3), *heavy), -limit, limit).astype(kind)


def setup_inputs(seed: int = 0) -> dict:
    key_of = jax.random.split(jax.random.key(seed), 16)
    cotangent = heavy_noise(key_of[0], (TOKENS, D), 1.0, 6.0, ((0, 4), (1, 8)), (0, 1, 8, 2.0))
    block_input = noise(key_of[1], (TOKENS, D), 1.0, 6.0, ((0, 4), (1, 8)))
    routes_keys = jax.random.split(jax.random.fold_in(key_of[2], 1), TOKENS // TOK_DEV)
    routes_turns = jax.random.permutation(jax.random.fold_in(key_of[2], 3), TOKENS // TOK_DEV)
    routes = jax.vmap(lambda own, number: routed_block(jax.random.fold_in(key_of[2], 2), own, number, TOK_DEV, EXPERTS, TOP_K, CAP, 2))(routes_keys, routes_turns).reshape((TOKENS, TOP_K))
    route_weights = jnp.clip(0.1 + 0.79999997 * jax.random.uniform(key_of[3], (TOKENS, TOP_K), jnp.float32) ** steps_of(key_of[3], (TOKENS, TOP_K), ((0, 4),), -0.2, 0.2), 0.1, 0.9)
    gate_weight = noise(key_of[4], (EXPERTS, D, FF), D ** -0.5, 0.125, ((0, 4), (2, 8)))
    up_weight = noise(key_of[5], (EXPERTS, D, FF), D ** -0.5, 0.125, ((0, 4), (2, 8)))
    down_weight = noise(key_of[6], (EXPERTS, FF, D), FF ** -0.5, 0.0625, ((0, 4), (1, 8)))
    out_weight = noise(key_of[7], (WIDTH, D), WIDTH ** -0.5, 0.1875, ((0, 8),))
    conv_out = noise(key_of[8], (WIDTH, TOKENS), 1.0, 6.0, ((0, 8), (1, 4)))
    gate_pre = noise(key_of[9], (WIDTH, TOKENS), 1.0, 6.0, ((0, 8), (1, 4)))
    prior_states = noise(key_of[10], (WIDTH, TOKENS), 1.0, 6.0, ((0, 8), (1, 4)))
    recur_weight = noise(key_of[11], (HEADS, HEAD_DIM, HEAD_DIM), HEAD_DIM ** -0.5, 0.75)
    input_gate_matrix = noise(key_of[12], (HEADS, HEAD_DIM, HEAD_DIM), HEAD_DIM ** -0.5, 0.75)
    decay_param = draw_decay_param(jax.random.fold_in(key_of[15], 71), 0)
    decay_jump = draw_decay_jump(jax.random.fold_in(key_of[15], 71), 0)
    return dict(cotangent=cotangent, block_input=block_input, routes=routes, route_weights=route_weights, gate_weight=gate_weight, up_weight=up_weight, down_weight=down_weight, out_weight=out_weight, conv_out=conv_out, gate_pre=gate_pre, prior_states=prior_states, recur_weight=recur_weight, input_gate_matrix=input_gate_matrix, decay_param=decay_param, decay_jump=decay_jump)


RATE_SCALE = 8.0

def link_pairs(left_pair, right_pair):
    return (left_pair[0] * right_pair[0], right_pair[0] * left_pair[1] + right_pair[1])

def expert_pass(operands, padded_input, padded_cot):
    index_row, weight_row, w_gate, w_up, w_down = operands
    slot_rows = padded_input[index_row]
    slot_cot = (weight_row[:, None] * padded_cot[index_row].astype(jnp.float32)).astype(jnp.bfloat16)
    gate_act = jnp.dot(slot_rows, w_gate, preferred_element_type=jnp.float32)
    up_act = jnp.dot(slot_rows, w_up, preferred_element_type=jnp.float32)
    sigma_gate = jax.nn.sigmoid(gate_act)
    silu_val = gate_act * sigma_gate
    hidden = (silu_val * up_act).astype(jnp.bfloat16)
    down_grad = jnp.dot(hidden.T, slot_cot, preferred_element_type=jnp.float32).astype(jnp.bfloat16)
    d_hidden = jnp.dot(slot_cot, w_down.T, preferred_element_type=jnp.float32)
    d_gate = (d_hidden * up_act * sigma_gate * (1.0 + gate_act * (1.0 - sigma_gate))).astype(jnp.bfloat16)
    d_up = (d_hidden * silu_val).astype(jnp.bfloat16)
    gate_grad = jnp.dot(slot_rows.T, d_gate, preferred_element_type=jnp.float32).astype(jnp.bfloat16)
    up_grad = jnp.dot(slot_rows.T, d_up, preferred_element_type=jnp.float32).astype(jnp.bfloat16)
    blocks = FF // N_TP
    row_count = index_row.shape[0]
    gate_parts = jnp.einsum('rnf,dnf->nrd', d_gate.astype(jnp.float32).reshape(row_count, N_TP, blocks), w_gate.astype(jnp.float32).reshape(D, N_TP, blocks))
    up_parts = jnp.einsum('rnf,dnf->nrd', d_up.astype(jnp.float32).reshape(row_count, N_TP, blocks), w_up.astype(jnp.float32).reshape(D, N_TP, blocks))
    width_part = lax.optimization_barrier((gate_parts + up_parts).astype(jnp.bfloat16))
    row_grad = lax.optimization_barrier(jnp.sum(width_part.astype(jnp.float32), axis=0)).astype(jnp.bfloat16)
    return (gate_grad, up_grad, down_grad, row_grad)

def reference(cotangent, block_input, routes, route_weights, gate_weight, up_weight, down_weight, out_weight, conv_out, gate_pre, prior_states, recur_weight, input_gate_matrix, decay_param, decay_jump):
    route_count = TOK_DEV * TOP_K
    flat_routes = routes.reshape(N_SP, route_count).astype(jnp.int32)
    onehot = (flat_routes[:, :, None] == jnp.arange(EXPERTS, dtype=jnp.int32)[None, None, :]).astype(jnp.int32)
    slot_rank = lax.optimization_barrier(jnp.sum((jnp.cumsum(onehot, axis=1) - onehot) * onehot, axis=2)).astype(jnp.int32)
    source = jnp.arange(N_SP, dtype=jnp.int32)[:, None]
    position = jnp.arange(route_count, dtype=jnp.int32)[None, :]
    token_ids = (source * TOK_DEV + position // TOP_K).astype(jnp.int32)
    slot_ids = ((flat_routes * N_SP + source) * CAP + slot_rank).astype(jnp.int32)
    total = EXPERTS * N_SP * CAP
    table = jnp.full((total,), TOKENS, jnp.int32).at[slot_ids.reshape(-1)].set(token_ids.reshape(-1))
    weight_table = jnp.zeros((total,), jnp.float32).at[slot_ids.reshape(-1)].set(route_weights.reshape(N_SP, route_count).reshape(-1))
    padded_input = jnp.concatenate([block_input, jnp.zeros((1, D), jnp.bfloat16)], axis=0)
    padded_cot = jnp.concatenate([cotangent, jnp.zeros((1, D), jnp.bfloat16)], axis=0)
    gate_weight_grad, up_weight_grad, down_weight_grad, row_grads = lax.map(partial_expert(padded_input, padded_cot), (table.reshape(EXPERTS, N_SP * CAP), weight_table.reshape(EXPERTS, N_SP * CAP), gate_weight, up_weight, down_weight))
    moe_grad = jnp.zeros((TOKENS + 1, D), jnp.float32).at[table].add(row_grads.reshape(total, D).astype(jnp.float32))[:TOKENS]
    block_grad = (cotangent.astype(jnp.float32) + moe_grad).astype(jnp.bfloat16)
    conv_vals = conv_out.astype(jnp.float32)
    shaped = conv_vals.reshape(HEADS, HEAD_DIM, TOKENS)
    recur_gate = jax.nn.sigmoid(jnp.einsum('hij,hit->hjt', recur_weight.astype(jnp.float32), shaped).reshape(WIDTH, TOKENS))
    input_gate = jax.nn.sigmoid(jnp.einsum('hij,hit->hjt', input_gate_matrix.astype(jnp.float32), shaped).reshape(WIDTH, TOKENS))
    softened = jax.nn.softplus(-decay_param)[:, None]
    log_decay = -RATE_SCALE * recur_gate * softened + decay_jump
    decay_val = jnp.exp(log_decay)
    norm_scale = jnp.sqrt(-jnp.expm1(2.0 * log_decay))
    prior_vals = prior_states.astype(jnp.float32)
    state = decay_val * prior_vals + norm_scale * input_gate * conv_vals
    gate_vals = gate_pre.astype(jnp.float32)
    gelu_val, gelu_pull = jax.vjp(jax.nn.gelu, gate_vals)
    mixed = (gelu_val * state).astype(jnp.bfloat16)
    out_weight_grad = jnp.dot(mixed, block_grad, preferred_element_type=jnp.float32)
    d_mixed = jnp.dot(out_weight, block_grad.T, preferred_element_type=jnp.float32)
    valve_logit_derivative = gelu_pull(d_mixed * state)[0].astype(jnp.bfloat16)
    d_state = d_mixed * gelu_val
    shifted = jnp.concatenate([decay_val[:, 1:], jnp.ones((WIDTH, 1), jnp.float32)], axis=1)
    flipped = lax.associative_scan(link_pairs, (jnp.flip(shifted, 1), jnp.flip(d_state, 1)), axis=1)
    state_grad = jnp.flip(flipped[1], 1)
    grad_log = state_grad * prior_vals * decay_val - state_grad * input_gate * conv_vals * decay_val * decay_val / norm_scale
    grad_recur = (grad_log * -RATE_SCALE * softened * recur_gate * (1.0 - recur_gate)).astype(jnp.bfloat16)
    grad_input = (state_grad * norm_scale * conv_vals * input_gate * (1.0 - input_gate)).astype(jnp.bfloat16)
    back_recur = jnp.einsum('hij,hjt->hit', recur_weight.astype(jnp.float32), grad_recur.astype(jnp.float32).reshape(HEADS, HEAD_DIM, TOKENS)).reshape(WIDTH, TOKENS)
    back_input = jnp.einsum('hij,hjt->hit', input_gate_matrix.astype(jnp.float32), grad_input.astype(jnp.float32).reshape(HEADS, HEAD_DIM, TOKENS)).reshape(WIDTH, TOKENS)
    conv_grad = (state_grad * norm_scale * input_gate + back_recur + back_input).astype(jnp.bfloat16)
    return (gate_weight_grad, up_weight_grad, down_weight_grad, out_weight_grad, conv_grad, valve_logit_derivative)

def partial_expert(padded_input, padded_cot):

    def run_expert(operands):
        return expert_pass(operands, padded_input, padded_cot)
    return run_expert
```

```python
import functools

import jax
import jax.numpy as jnp
from jax import lax
from jax.experimental import pallas as pl
from jax.experimental.pallas import tpu as pltpu
from jax.sharding import PartitionSpec as P

HEAD_DIM = 64
TOP_K = 2


RATE_SCALE = 8.0


def link_pairs(left_pair, right_pair):
    return (left_pair[0] * right_pair[0], right_pair[0] * left_pair[1] + right_pair[1])


def routing_tables(routes, experts, capacity):
    flat_routes = routes.reshape(-1)
    onehot = (flat_routes[:, None] == jnp.arange(experts, dtype=jnp.int32)[None, :]).astype(
        jnp.int32
    )
    slot_rank = jnp.sum((jnp.cumsum(onehot, axis=0) - onehot) * onehot, axis=1)
    target = (flat_routes * capacity + slot_rank).reshape(routes.shape[0], routes.shape[1])
    slot_ids = jnp.arange(experts * capacity, dtype=jnp.int32)
    return jnp.transpose(target)[:, None, :] == slot_ids[None, :, None]


CORES = 2
VMEM = pl.BlockSpec(memory_space=pltpu.VMEM)


def across(place, step, size):
    result, bit = 0, 1
    while bit < size:
        result = result + lax.rem(lax.div(place, bit) + (step // bit) % 2, 2) * bit
        bit *= 2
    return result


def send(source, target, sems, index, device):
    return pltpu.make_async_remote_copy(
        src_ref=source,
        dst_ref=target,
        send_sem=sems[0].at[index],
        recv_sem=sems[1].at[index],
        device_id=device,
        device_id_type=pl.DeviceIdType.MESH,
    )


def greet(devices):
    barrier = pltpu.get_barrier_semaphore()
    for device in devices:
        pl.semaphore_signal(
            barrier, inc=1, device_id=device, device_id_type=pl.DeviceIdType.MESH
        )
    pl.semaphore_wait(barrier, len(devices))


def position(deep):
    sp, tp = lax.axis_index("sp"), lax.axis_index("tp")
    z, core = lax.div(tp, CORES), lax.rem(tp, CORES)
    return sp, tp, z, core, (sp, z * CORES + 1 - core)


def columns(block, width):
    return pl.ds(pl.multiple_of(block * width, width), width)


def dispatch_kernel(
    experts,
    deep,
    rows_in,
    cot_in,
    placing,
    slot_weight,
    rows_out,
    cot_out,
    held,
    stage,
    z_send,
    z_recv,
    p_send,
    p_recv,
    c_send,
    c_recv,
):
    sp, tp, z, core, partner = position(deep)
    width = rows_in.shape[1]
    planes = [(across(sp, k, experts), tp) for k in range(experts)]
    levels = [across(z, d, deep) for d in range(deep)]
    lines = [(sp, level * CORES + core) for level in levels]
    greet(planes[1:] + lines[1:] + [partner])
    sources, outs = (rows_in, cot_in), (rows_out, cot_out)
    line_copies, plane_copies = {}, {}
    for a in range(2):
        for d in range(1, deep):
            copy = send(sources[a], held.at[a, d - 1], (z_send, z_recv), (a, d), lines[d])
            copy.start()
            line_copies[a, d] = copy
    for a in range(2):
        for d in range(deep):
            if d:
                line_copies[a, d].wait_recv()
            block = held[a, d - 1] if d else sources[a][...]
            here = columns(levels[d] * CORES + core, width)
            for k in list(range(1, experts)) + [0]:
                expert = planes[k][0]
                piece = jnp.dot(placing[expert], block, preferred_element_type=jnp.float32)
                if a:
                    piece = piece * slot_weight[expert]
                piece = piece.astype(jnp.bfloat16)
                if k == 0:
                    outs[a][sp, :, here] = piece
                else:
                    stage[a, d, k - 1] = piece
                    copy = send(
                        stage.at[a, d, k - 1],
                        outs[a].at[sp, :, here],
                        (p_send, p_recv),
                        (a, d, k),
                        planes[k],
                    )
                    copy.start()
                    plane_copies[a, d, k] = copy
    core_copies = []
    for a in range(2):
        for d in range(deep):
            for k in range(1, experts):
                plane_copies[a, d, k].wait_recv()
            here = columns(levels[d] * CORES + core, width)
            copy = send(
                outs[a].at[:, :, here], outs[a].at[:, :, here], (c_send, c_recv), (a, d), partner
            )
            copy.start()
            core_copies.append(copy)
    for copy in core_copies:
        copy.wait_recv()
    for copy in core_copies + list(plane_copies.values()) + list(line_copies.values()):
        copy.wait_send()


def dispatch(rows_in, cot_in, placing, slot_weight):
    experts, capacity, tok_rows = placing.shape
    deep = lax.axis_size("tp") // CORES
    width = rows_in.shape[1]
    out = jax.ShapeDtypeStruct((experts, capacity, width * deep * CORES), jnp.bfloat16)
    sems = [(2, deep), (2, deep, experts), (2, deep)]
    return pl.pallas_call(
        functools.partial(dispatch_kernel, experts, deep),
        out_shape=(out, out),
        in_specs=[VMEM] * 4,
        out_specs=(VMEM, VMEM),
        scratch_shapes=[
            pltpu.VMEM((2, deep - 1, tok_rows, width), jnp.bfloat16),
            pltpu.VMEM((2, deep, experts - 1, capacity, width), jnp.bfloat16),
        ]
        + [pltpu.SemaphoreType.DMA(shape) for shape in sems for _ in range(2)],
        compiler_params=pltpu.CompilerParams(
            collective_id=0, has_side_effects=True, vmem_limit_bytes=48 << 20
        ),
    )(rows_in, cot_in, placing, slot_weight)


def combine_kernel(
    experts,
    deep,
    parts,
    cot_in,
    taking,
    full_out,
    paired,
    stage,
    plane,
    line_out,
    line_in,
    c_send,
    c_recv,
    p_send,
    p_recv,
    z_send,
    z_recv,
    g_send,
    g_recv,
    f_send,
    f_recv,
):
    sp, tp, z, core, partner = position(deep)
    width = cot_in.shape[1]
    planes = [(across(sp, k, experts), tp) for k in range(experts)]
    levels = [across(z, d, deep) for d in range(deep)]
    lines = [(sp, level * CORES + core) for level in levels]
    greet(planes[1:] + lines[1:] + [partner])
    order = list(range(deep - 1, -1, -1))
    started, core_copies, plane_copies, line_copies = [], {}, {}, {}
    for d in order:
        theirs = columns(levels[d] * CORES + 1 - core, width)
        copy = send(parts.at[:, :, theirs], paired.at[d], (c_send, c_recv), d, partner)
        copy.start()
        core_copies[d] = copy
        started.append(copy)
    for d in order:
        core_copies[d].wait_recv()
        here = columns(levels[d] * CORES + core, width)
        for k in list(range(1, experts)) + [0]:
            home = planes[k][0]
            piece = (
                parts[home, :, here].astype(jnp.float32) + paired[d, home].astype(jnp.float32)
            ).astype(jnp.bfloat16)
            if k == 0:
                plane[d, 0] = piece
            else:
                stage[d, k - 1] = piece
                copy = send(
                    stage.at[d, k - 1], plane.at[d, k], (p_send, p_recv), (d, k), planes[k]
                )
                copy.start()
                plane_copies[d, k] = copy
                started.append(copy)
    total = cot_in[...].astype(jnp.float32)
    for d in order:
        summed = jnp.dot(taking[sp], plane[d, 0], preferred_element_type=jnp.float32)
        for k in range(1, experts):
            plane_copies[d, k].wait_recv()
            summed = summed + jnp.dot(
                taking[planes[k][0]], plane[d, k], preferred_element_type=jnp.float32
            )
        if d == 0:
            total = total + summed
        else:
            line_out[d - 1] = summed.astype(jnp.bfloat16)
            copy = send(line_out.at[d - 1], line_in.at[d - 1], (z_send, z_recv), d, lines[d])
            copy.start()
            line_copies[d] = copy
            started.append(copy)
    for d in order[:-1]:
        line_copies[d].wait_recv()
        total = total + line_in[d - 1].astype(jnp.float32)
    mine = columns(tp, width)
    full_out[:, mine] = total.astype(jnp.bfloat16)
    gathers, forwards = {}, []
    for d in range(1, deep):
        copy = send(full_out.at[:, mine], full_out.at[:, mine], (g_send, g_recv), d, lines[d])
        copy.start()
        gathers[d] = copy
        started.append(copy)
    for d in range(deep):
        if d:
            gathers[d].wait_recv()
        here = columns(levels[d] * CORES + core, width)
        copy = send(full_out.at[:, here], full_out.at[:, here], (f_send, f_recv), d, partner)
        copy.start()
        forwards.append(copy)
    for copy in forwards:
        copy.wait_recv()
    for copy in started + forwards:
        copy.wait_send()


def combine(parts, cot_in, taking):
    experts, capacity, full_width = parts.shape
    tok_rows, width = cot_in.shape
    deep = lax.axis_size("tp") // CORES
    sems = [(deep,), (deep, experts), (deep,), (deep,), (deep,)]
    return pl.pallas_call(
        functools.partial(combine_kernel, experts, deep),
        out_shape=jax.ShapeDtypeStruct((tok_rows, full_width), jnp.bfloat16),
        in_specs=[VMEM] * 3,
        out_specs=VMEM,
        scratch_shapes=[
            pltpu.VMEM((deep, experts, capacity, width), jnp.bfloat16),
            pltpu.VMEM((deep, experts - 1, capacity, width), jnp.bfloat16),
            pltpu.VMEM((deep, experts, capacity, width), jnp.bfloat16),
            pltpu.VMEM((deep - 1, tok_rows, width), jnp.bfloat16),
            pltpu.VMEM((deep - 1, tok_rows, width), jnp.bfloat16),
        ]
        + [pltpu.SemaphoreType.DMA(shape) for shape in sems for _ in range(2)],
        compiler_params=pltpu.CompilerParams(
            collective_id=1, has_side_effects=True, vmem_limit_bytes=48 << 20
        ),
    )(parts, cot_in, taking)


def closing_kernel(
    count, summary, product, summaries, products, s_send, s_recv, p_send, p_recv
):
    sp, tp = lax.axis_index("sp"), lax.axis_index("tp")
    width = products.shape[2]
    peers = [(across(sp, k, count), tp) for k in range(count)]
    greet(peers[1:])
    copies = []
    for k in range(1, count):
        copies.append(send(summary, summaries.at[sp], (s_send, s_recv), k, peers[k]))
        copies[-1].start()
    for k in range(1, count):
        theirs = columns(peers[k][0], width)
        copies.append(
            send(product.at[:, theirs], products.at[k], (p_send, p_recv), k, peers[k])
        )
        copies[-1].start()
    summaries[sp] = summary[...]
    products[0] = product[:, columns(sp, width)]
    for copy in copies:
        copy.wait()


def closing(summary, product):
    count = lax.axis_size("sp")
    channels, full_width = product.shape
    return pl.pallas_call(
        functools.partial(closing_kernel, count),
        out_shape=(
            jax.ShapeDtypeStruct((count,) + summary.shape, summary.dtype),
            jax.ShapeDtypeStruct((count, channels, full_width // count), product.dtype),
        ),
        in_specs=[VMEM] * 2,
        out_specs=(VMEM, VMEM),
        scratch_shapes=[pltpu.SemaphoreType.DMA((count,)) for _ in range(4)],
        compiler_params=pltpu.CompilerParams(
            collective_id=2, has_side_effects=True, vmem_limit_bytes=16 << 20
        ),
    )(summary, product)


def expert_work(slot_rows, slot_cot, w_gate, w_up, w_down):
    minor = (((1,), (1,)), ((), ()))
    gate_act = jnp.dot(slot_rows, w_gate, preferred_element_type=jnp.float32)
    up_act = jnp.dot(slot_rows, w_up, preferred_element_type=jnp.float32)
    sigma_gate = jax.nn.sigmoid(gate_act)
    silu_val = gate_act * sigma_gate
    hidden = (silu_val * up_act).astype(jnp.bfloat16)
    d_hidden = lax.dot_general(slot_cot, w_down, minor, preferred_element_type=jnp.float32)
    d_gate = (d_hidden * up_act * sigma_gate * (1.0 + gate_act * (1.0 - sigma_gate))).astype(
        jnp.bfloat16
    )
    d_up = (d_hidden * silu_val).astype(jnp.bfloat16)
    width_part = lax.dot_general(d_gate, w_gate, minor, preferred_element_type=jnp.float32)
    width_part = width_part + lax.dot_general(d_up, w_up, minor, preferred_element_type=jnp.float32)
    return (hidden, d_gate, d_up, width_part)


def weight_grads(slot_rows, slot_cot, hidden, d_gate, d_up):
    major = (((0,), (0,)), ((), ()))
    gate_grad = lax.dot_general(
        slot_rows, d_gate, major, preferred_element_type=jnp.float32
    ).astype(jnp.bfloat16)
    up_grad = lax.dot_general(slot_rows, d_up, major, preferred_element_type=jnp.float32).astype(
        jnp.bfloat16
    )
    down_grad = lax.dot_general(hidden, slot_cot, major, preferred_element_type=jnp.float32).astype(
        jnp.bfloat16
    )
    return (gate_grad[None], up_grad[None], down_grad[None])


def local(
    cotangent,
    block_input,
    routes,
    route_weights,
    gate_weight,
    up_weight,
    down_weight,
    out_weight,
    conv_out,
    gate_pre,
    prior_states,
    recur_weight,
    input_gate_matrix,
    decay_param,
    decay_jump,
):
    experts = lax.axis_size("sp")
    tok_rows = cotangent.shape[0]
    capacity = 5 * tok_rows * TOP_K // (4 * experts)
    route_hits = routing_tables(routes, experts, capacity)
    hits = jnp.sum(route_hits.astype(jnp.float32), axis=0)
    placing = hits.astype(jnp.bfloat16).reshape(experts, capacity, tok_rows)
    taking = jnp.swapaxes(placing, 1, 2)
    slot_weight = jnp.sum(
        jnp.where(route_hits, jnp.transpose(route_weights)[:, None, :], 0.0), axis=(0, 2)
    ).reshape(experts, capacity, 1)
    got_rows, got_cot = dispatch(block_input, cotangent, placing, slot_weight)
    full_width = got_rows.shape[2]
    slot_rows = got_rows.reshape(-1, full_width)
    slot_cot = got_cot.reshape(-1, full_width)
    hidden, d_gate, d_up, width_part = expert_work(
        slot_rows, slot_cot, gate_weight[0], up_weight[0], down_weight[0]
    )
    gate_grad, up_grad, down_grad = weight_grads(slot_rows, slot_cot, hidden, d_gate, d_up)
    full_grad = combine(
        width_part.astype(jnp.bfloat16).reshape(experts, capacity, full_width), cotangent, taking
    )
    channels = conv_out.shape[0]
    length = conv_out.shape[1]
    head_count = channels // HEAD_DIM
    head_start = lax.axis_index("tp") * head_count
    w_recur = lax.dynamic_slice_in_dim(recur_weight, head_start, head_count, 0)
    w_input = lax.dynamic_slice_in_dim(input_gate_matrix, head_start, head_count, 0)
    rate_parameter = lax.dynamic_slice_in_dim(decay_param, head_start * HEAD_DIM, channels, 0)[
        :, None
    ]
    shaped = conv_out.reshape(head_count, HEAD_DIM, length)
    recur_gate = jax.nn.sigmoid(
        jnp.einsum("hij,hit->hjt", w_recur, shaped, preferred_element_type=jnp.float32).reshape(
            channels, length
        )
    )
    input_gate = jax.nn.sigmoid(
        jnp.einsum("hij,hit->hjt", w_input, shaped, preferred_element_type=jnp.float32).reshape(
            channels, length
        )
    )
    softened = jax.nn.softplus(-rate_parameter)
    log_decay = -RATE_SCALE * recur_gate * softened + decay_jump
    decay_val = jnp.exp(log_decay)
    norm_scale = jnp.sqrt(-jnp.expm1(2.0 * log_decay))
    conv_vals = conv_out.astype(jnp.float32)
    prior_vals = prior_states.astype(jnp.float32)
    state = decay_val * prior_vals + norm_scale * input_gate * conv_vals
    gelu_val, gelu_pull = jax.vjp(jax.nn.gelu, gate_pre.astype(jnp.float32))
    mixed = (gelu_val * state).astype(jnp.bfloat16)
    d_mixed = lax.dot_general(
        out_weight, full_grad, (((1,), (1,)), ((), ())), preferred_element_type=jnp.float32
    )
    valve_logit_derivative = gelu_pull(d_mixed * state)[0].astype(jnp.bfloat16)
    d_state = d_mixed * gelu_val
    shifted = jnp.concatenate([decay_val[:, 1:], jnp.ones((channels, 1), jnp.float32)], axis=1)
    flipped = lax.associative_scan(link_pairs, (jnp.flip(shifted, 1), jnp.flip(d_state, 1)), axis=1)
    decay_prod = jnp.flip(flipped[0], 1)
    local_sum = jnp.flip(flipped[1], 1)
    summary = jnp.stack([decay_val[:, 0] * decay_prod[:, 0], decay_val[:, 0] * local_sum[:, 0]])
    product = jnp.dot(mixed, full_grad, preferred_element_type=jnp.float32).astype(jnp.bfloat16)
    summaries, products = closing(summary, product)
    carried = jnp.zeros((channels,), jnp.float32)
    for later in range(experts - 1, 0, -1):
        longer = summaries[later, 1] + summaries[later, 0] * carried
        carried = jnp.where(later > lax.axis_index("sp"), longer, carried)
    out_weight_grad = jnp.sum(products.astype(jnp.float32), axis=0)
    state_grad = local_sum + decay_prod * carried[:, None]
    grad_log = (
        state_grad * prior_vals * decay_val
        - state_grad * input_gate * conv_vals * decay_val * decay_val / norm_scale
    )
    grad_recur = (grad_log * -RATE_SCALE * softened * recur_gate * (1.0 - recur_gate)).astype(
        jnp.bfloat16
    )
    grad_input = (state_grad * norm_scale * conv_vals * input_gate * (1.0 - input_gate)).astype(
        jnp.bfloat16
    )
    back_recur = jnp.einsum(
        "hij,hjt->hit",
        w_recur,
        grad_recur.reshape(head_count, HEAD_DIM, length),
        preferred_element_type=jnp.float32,
    ).reshape(channels, length)
    back_input = jnp.einsum(
        "hij,hjt->hit",
        w_input,
        grad_input.reshape(head_count, HEAD_DIM, length),
        preferred_element_type=jnp.float32,
    ).reshape(channels, length)
    conv_grad = (state_grad * norm_scale * input_gate + back_recur + back_input).astype(
        jnp.bfloat16
    )
    return (gate_grad, up_grad, down_grad, out_weight_grad, conv_grad, valve_logit_derivative)


def solution(mesh):
    in_specs = (
        P("sp", "tp"),
        P("sp", "tp"),
        P("sp", None),
        P("sp", None),
        P("sp", None, "tp"),
        P("sp", None, "tp"),
        P("sp", "tp", None),
        P("tp", None),
        P("tp", "sp"),
        P("tp", "sp"),
        P("tp", "sp"),
        P(),
        P(),
        P(),
        P("tp", "sp"),
    )
    out_specs = (
        P("sp", None, "tp"),
        P("sp", None, "tp"),
        P("sp", "tp", None),
        P("tp", "sp"),
        P("tp", "sp"),
        P("tp", "sp"),
    )
    return jax.shard_map(local, mesh=mesh, in_specs=in_specs, out_specs=out_specs, check_vma=False)
```

```python
import functools

import jax
import jax.numpy as jnp
from jax import lax
from jax.experimental import pallas as pl
from jax.experimental.pallas import tpu as pltpu
from jax.sharding import PartitionSpec as P

HEAD_DIM = 64
TOP_K = 2


RATE_SCALE = 8.0


def link_pairs(left_pair, right_pair):
    return (left_pair[0] * right_pair[0], right_pair[0] * left_pair[1] + right_pair[1])


def routing_tables(routes, experts, capacity):
    flat_routes = routes.reshape(-1)
    onehot = (flat_routes[:, None] == jnp.arange(experts, dtype=jnp.int32)[None, :]).astype(
        jnp.int32
    )
    slot_rank = jnp.sum((jnp.cumsum(onehot, axis=0) - onehot) * onehot, axis=1)
    target = (flat_routes * capacity + slot_rank).reshape(routes.shape[0], routes.shape[1])
    slot_ids = jnp.arange(experts * capacity, dtype=jnp.int32)
    return jnp.transpose(target)[:, None, :] == slot_ids[None, :, None]


CORES = 2
VMEM = pl.BlockSpec(memory_space=pltpu.VMEM)


def across(place, step, size):
    result, bit = 0, 1
    while bit < size:
        result = result + lax.rem(lax.div(place, bit) + (step // bit) % 2, 2) * bit
        bit *= 2
    return result


def send(source, target, sems, index, device):
    return pltpu.make_async_remote_copy(
        src_ref=source,
        dst_ref=target,
        send_sem=sems[0].at[index],
        recv_sem=sems[1].at[index],
        device_id=device,
        device_id_type=pl.DeviceIdType.MESH,
    )


def greet(devices):
    barrier = pltpu.get_barrier_semaphore()
    for device in devices:
        pl.semaphore_signal(
            barrier, inc=1, device_id=device, device_id_type=pl.DeviceIdType.MESH
        )
    pl.semaphore_wait(barrier, len(devices))


def position(deep):
    sp, tp = lax.axis_index("sp"), lax.axis_index("tp")
    z, core = lax.div(tp, CORES), lax.rem(tp, CORES)
    return sp, tp, z, core, (sp, z * CORES + 1 - core)


def columns(block, width):
    return pl.ds(pl.multiple_of(block * width, width), width)


def dispatch_kernel(
    experts,
    deep,
    rows_in,
    cot_in,
    placing,
    slot_weight,
    rows_out,
    cot_out,
    held,
    stage,
    z_send,
    z_recv,
    p_send,
    p_recv,
    c_send,
    c_recv,
):
    sp, tp, z, core, partner = position(deep)
    width = rows_in.shape[1]
    planes = [(across(sp, k, experts), tp) for k in range(experts)]
    levels = [across(z, d, deep) for d in range(deep)]
    lines = [(sp, level * CORES + core) for level in levels]
    greet(planes[1:] + lines[1:] + [partner])
    sources, outs = (rows_in, cot_in), (rows_out, cot_out)
    line_copies, plane_copies = {}, {}
    for a in range(2):
        for d in range(1, deep):
            copy = send(sources[a], held.at[a, d - 1], (z_send, z_recv), (a, d), lines[d])
            copy.start()
            line_copies[a, d] = copy
    own_first = [(0, 0), (1, 0)] + [(a, d) for a in range(2) for d in range(1, deep)]
    for a, d in own_first:
            if d:
                line_copies[a, d].wait_recv()
            block = held[a, d - 1] if d else sources[a][...]
            here = columns(levels[d] * CORES + core, width)
            for k in list(range(1, experts)) + [0]:
                expert = planes[k][0]
                piece = jnp.dot(placing[expert], block, preferred_element_type=jnp.float32)
                if a:
                    piece = piece * slot_weight[expert]
                piece = piece.astype(jnp.bfloat16)
                if k == 0:
                    outs[a][sp, :, here] = piece
                else:
                    stage[a, d, k - 1] = piece
                    copy = send(
                        stage.at[a, d, k - 1],
                        outs[a].at[sp, :, here],
                        (p_send, p_recv),
                        (a, d, k),
                        planes[k],
                    )
                    copy.start()
                    plane_copies[a, d, k] = copy
    core_copies = []
    for a in range(2):
        for d in range(deep):
            for k in range(1, experts):
                plane_copies[a, d, k].wait_recv()
            here = columns(levels[d] * CORES + core, width)
            copy = send(
                outs[a].at[:, :, here], outs[a].at[:, :, here], (c_send, c_recv), (a, d), partner
            )
            copy.start()
            core_copies.append(copy)
    for copy in core_copies:
        copy.wait_recv()
    for copy in core_copies + list(plane_copies.values()) + list(line_copies.values()):
        copy.wait_send()


def dispatch(rows_in, cot_in, placing, slot_weight):
    experts, capacity, tok_rows = placing.shape
    deep = lax.axis_size("tp") // CORES
    width = rows_in.shape[1]
    out = jax.ShapeDtypeStruct((experts, capacity, width * deep * CORES), jnp.bfloat16)
    sems = [(2, deep), (2, deep, experts), (2, deep)]
    return pl.pallas_call(
        functools.partial(dispatch_kernel, experts, deep),
        out_shape=(out, out),
        in_specs=[VMEM] * 4,
        out_specs=(VMEM, VMEM),
        scratch_shapes=[
            pltpu.VMEM((2, deep - 1, tok_rows, width), jnp.bfloat16),
            pltpu.VMEM((2, deep, experts - 1, capacity, width), jnp.bfloat16),
        ]
        + [pltpu.SemaphoreType.DMA(shape) for shape in sems for _ in range(2)],
        compiler_params=pltpu.CompilerParams(
            collective_id=0, has_side_effects=True, vmem_limit_bytes=48 << 20
        ),
    )(rows_in, cot_in, placing, slot_weight)


def combine_kernel(
    experts,
    deep,
    parts,
    cot_in,
    taking,
    full_out,
    paired,
    stage,
    plane,
    line_out,
    line_in,
    c_send,
    c_recv,
    p_send,
    p_recv,
    z_send,
    z_recv,
    g_send,
    g_recv,
    f_send,
    f_recv,
):
    sp, tp, z, core, partner = position(deep)
    width = cot_in.shape[1]
    planes = [(across(sp, k, experts), tp) for k in range(experts)]
    levels = [across(z, d, deep) for d in range(deep)]
    lines = [(sp, level * CORES + core) for level in levels]
    greet(planes[1:] + lines[1:] + [partner])
    order = list(range(deep - 1, -1, -1))
    started, core_copies, plane_copies, line_copies = [], {}, {}, {}
    for d in order:
        theirs = columns(levels[d] * CORES + 1 - core, width)
        copy = send(parts.at[:, :, theirs], paired.at[d], (c_send, c_recv), d, partner)
        copy.start()
        core_copies[d] = copy
        started.append(copy)
    for d in order:
        core_copies[d].wait_recv()
        here = columns(levels[d] * CORES + core, width)
        for k in list(range(1, experts)) + [0]:
            home = planes[k][0]
            piece = (
                parts[home, :, here].astype(jnp.float32) + paired[d, home].astype(jnp.float32)
            ).astype(jnp.bfloat16)
            if k == 0:
                plane[d, 0] = piece
            else:
                stage[d, k - 1] = piece
                copy = send(
                    stage.at[d, k - 1], plane.at[d, k], (p_send, p_recv), (d, k), planes[k]
                )
                copy.start()
                plane_copies[d, k] = copy
                started.append(copy)
    total = cot_in[...].astype(jnp.float32)
    for d in order:
        summed = jnp.dot(taking[sp], plane[d, 0], preferred_element_type=jnp.float32)
        for k in range(1, experts):
            plane_copies[d, k].wait_recv()
            summed = summed + jnp.dot(
                taking[planes[k][0]], plane[d, k], preferred_element_type=jnp.float32
            )
        if d == 0:
            total = total + summed
        else:
            line_out[d - 1] = summed.astype(jnp.bfloat16)
            copy = send(line_out.at[d - 1], line_in.at[d - 1], (z_send, z_recv), d, lines[d])
            copy.start()
            line_copies[d] = copy
            started.append(copy)
    for d in order[:-1]:
        line_copies[d].wait_recv()
        total = total + line_in[d - 1].astype(jnp.float32)
    mine = columns(tp, width)
    full_out[:, mine] = total.astype(jnp.bfloat16)
    gathers, forwards = {}, []
    for d in range(1, deep):
        copy = send(full_out.at[:, mine], full_out.at[:, mine], (g_send, g_recv), d, lines[d])
        copy.start()
        gathers[d] = copy
        started.append(copy)
    for d in range(deep):
        if d:
            gathers[d].wait_recv()
        here = columns(levels[d] * CORES + core, width)
        copy = send(full_out.at[:, here], full_out.at[:, here], (f_send, f_recv), d, partner)
        copy.start()
        forwards.append(copy)
    for copy in forwards:
        copy.wait_recv()
    for copy in started + forwards:
        copy.wait_send()


def combine(parts, cot_in, taking):
    experts, capacity, full_width = parts.shape
    tok_rows, width = cot_in.shape
    deep = lax.axis_size("tp") // CORES
    sems = [(deep,), (deep, experts), (deep,), (deep,), (deep,)]
    return pl.pallas_call(
        functools.partial(combine_kernel, experts, deep),
        out_shape=jax.ShapeDtypeStruct((tok_rows, full_width), jnp.bfloat16),
        in_specs=[VMEM] * 3,
        out_specs=VMEM,
        scratch_shapes=[
            pltpu.VMEM((deep, experts, capacity, width), jnp.bfloat16),
            pltpu.VMEM((deep, experts - 1, capacity, width), jnp.bfloat16),
            pltpu.VMEM((deep, experts, capacity, width), jnp.bfloat16),
            pltpu.VMEM((deep - 1, tok_rows, width), jnp.bfloat16),
            pltpu.VMEM((deep - 1, tok_rows, width), jnp.bfloat16),
        ]
        + [pltpu.SemaphoreType.DMA(shape) for shape in sems for _ in range(2)],
        compiler_params=pltpu.CompilerParams(
            collective_id=1, has_side_effects=True, vmem_limit_bytes=48 << 20
        ),
    )(parts, cot_in, taking)


def closing_kernel(
    count, summary, product, summaries, products, s_send, s_recv, p_send, p_recv
):
    sp, tp = lax.axis_index("sp"), lax.axis_index("tp")
    width = products.shape[2]
    peers = [(across(sp, k, count), tp) for k in range(count)]
    greet(peers[1:])
    copies = []
    for k in range(1, count):
        copies.append(send(summary, summaries.at[sp], (s_send, s_recv), k, peers[k]))
        copies[-1].start()
    for k in range(1, count):
        theirs = columns(peers[k][0], width)
        copies.append(
            send(product.at[:, theirs], products.at[k], (p_send, p_recv), k, peers[k])
        )
        copies[-1].start()
    summaries[sp] = summary[...]
    products[0] = product[:, columns(sp, width)]
    for copy in copies:
        copy.wait()


def closing(summary, product):
    count = lax.axis_size("sp")
    channels, full_width = product.shape
    return pl.pallas_call(
        functools.partial(closing_kernel, count),
        out_shape=(
            jax.ShapeDtypeStruct((count,) + summary.shape, summary.dtype),
            jax.ShapeDtypeStruct((count, channels, full_width // count), product.dtype),
        ),
        in_specs=[VMEM] * 2,
        out_specs=(VMEM, VMEM),
        scratch_shapes=[pltpu.SemaphoreType.DMA((count,)) for _ in range(4)],
        compiler_params=pltpu.CompilerParams(
            collective_id=2, has_side_effects=True, vmem_limit_bytes=16 << 20
        ),
    )(summary, product)


def expert_work(slot_rows, slot_cot, w_gate, w_up, w_down):
    minor = (((1,), (1,)), ((), ()))
    gate_act = jnp.dot(slot_rows, w_gate, preferred_element_type=jnp.float32)
    up_act = jnp.dot(slot_rows, w_up, preferred_element_type=jnp.float32)
    sigma_gate = jax.nn.sigmoid(gate_act)
    silu_val = gate_act * sigma_gate
    hidden = (silu_val * up_act).astype(jnp.bfloat16)
    d_hidden = lax.dot_general(slot_cot, w_down, minor, preferred_element_type=jnp.float32)
    d_gate = (d_hidden * up_act * sigma_gate * (1.0 + gate_act * (1.0 - sigma_gate))).astype(
        jnp.bfloat16
    )
    d_up = (d_hidden * silu_val).astype(jnp.bfloat16)
    width_part = lax.dot_general(d_gate, w_gate, minor, preferred_element_type=jnp.float32)
    width_part = width_part + lax.dot_general(d_up, w_up, minor, preferred_element_type=jnp.float32)
    return (hidden, d_gate, d_up, width_part)


def weight_grads(slot_rows, slot_cot, hidden, d_gate, d_up):
    major = (((0,), (0,)), ((), ()))
    gate_grad = lax.dot_general(
        slot_rows, d_gate, major, preferred_element_type=jnp.float32
    ).astype(jnp.bfloat16)
    up_grad = lax.dot_general(slot_rows, d_up, major, preferred_element_type=jnp.float32).astype(
        jnp.bfloat16
    )
    down_grad = lax.dot_general(hidden, slot_cot, major, preferred_element_type=jnp.float32).astype(
        jnp.bfloat16
    )
    return (gate_grad[None], up_grad[None], down_grad[None])


def local(
    cotangent,
    block_input,
    routes,
    route_weights,
    gate_weight,
    up_weight,
    down_weight,
    out_weight,
    conv_out,
    gate_pre,
    prior_states,
    recur_weight,
    input_gate_matrix,
    decay_param,
    decay_jump,
):
    experts = lax.axis_size("sp")
    tok_rows = cotangent.shape[0]
    capacity = 5 * tok_rows * TOP_K // (4 * experts)
    route_hits = routing_tables(routes, experts, capacity)
    hits = jnp.sum(route_hits.astype(jnp.float32), axis=0)
    placing = hits.astype(jnp.bfloat16).reshape(experts, capacity, tok_rows)
    taking = jnp.swapaxes(placing, 1, 2)
    slot_weight = jnp.sum(
        jnp.where(route_hits, jnp.transpose(route_weights)[:, None, :], 0.0), axis=(0, 2)
    ).reshape(experts, capacity, 1)
    got_rows, got_cot = dispatch(block_input, cotangent, placing, slot_weight)
    full_width = got_rows.shape[2]
    slot_rows = got_rows.reshape(-1, full_width)
    slot_cot = got_cot.reshape(-1, full_width)
    hidden, d_gate, d_up, width_part = expert_work(
        slot_rows, slot_cot, gate_weight[0], up_weight[0], down_weight[0]
    )
    gate_grad, up_grad, down_grad = weight_grads(slot_rows, slot_cot, hidden, d_gate, d_up)
    full_grad = combine(
        width_part.astype(jnp.bfloat16).reshape(experts, capacity, full_width), cotangent, taking
    )
    channels = conv_out.shape[0]
    length = conv_out.shape[1]
    head_count = channels // HEAD_DIM
    head_start = lax.axis_index("tp") * head_count
    w_recur = lax.dynamic_slice_in_dim(recur_weight, head_start, head_count, 0)
    w_input = lax.dynamic_slice_in_dim(input_gate_matrix, head_start, head_count, 0)
    rate_parameter = lax.dynamic_slice_in_dim(decay_param, head_start * HEAD_DIM, channels, 0)[
        :, None
    ]
    shaped = conv_out.reshape(head_count, HEAD_DIM, length)
    recur_gate = jax.nn.sigmoid(
        jnp.einsum("hij,hit->hjt", w_recur, shaped, preferred_element_type=jnp.float32).reshape(
            channels, length
        )
    )
    input_gate = jax.nn.sigmoid(
        jnp.einsum("hij,hit->hjt", w_input, shaped, preferred_element_type=jnp.float32).reshape(
            channels, length
        )
    )
    softened = jax.nn.softplus(-rate_parameter)
    log_decay = -RATE_SCALE * recur_gate * softened + decay_jump
    decay_val = jnp.exp(log_decay)
    norm_scale = jnp.sqrt(-jnp.expm1(2.0 * log_decay))
    conv_vals = conv_out.astype(jnp.float32)
    prior_vals = prior_states.astype(jnp.float32)
    state = decay_val * prior_vals + norm_scale * input_gate * conv_vals
    gelu_val, gelu_pull = jax.vjp(jax.nn.gelu, gate_pre.astype(jnp.float32))
    mixed = (gelu_val * state).astype(jnp.bfloat16)
    d_mixed = lax.dot_general(
        out_weight, full_grad, (((1,), (1,)), ((), ())), preferred_element_type=jnp.float32
    )
    valve_logit_derivative = gelu_pull(d_mixed * state)[0].astype(jnp.bfloat16)
    d_state = d_mixed * gelu_val
    shifted = jnp.concatenate([decay_val[:, 1:], jnp.ones((channels, 1), jnp.float32)], axis=1)
    flipped = lax.associative_scan(link_pairs, (jnp.flip(shifted, 1), jnp.flip(d_state, 1)), axis=1)
    decay_prod = jnp.flip(flipped[0], 1)
    local_sum = jnp.flip(flipped[1], 1)
    summary = jnp.stack([decay_val[:, 0] * decay_prod[:, 0], decay_val[:, 0] * local_sum[:, 0]])
    product = jnp.dot(mixed, full_grad, preferred_element_type=jnp.float32).astype(jnp.bfloat16)
    summaries, products = closing(summary, product)
    carried = jnp.zeros((channels,), jnp.float32)
    for later in range(experts - 1, 0, -1):
        longer = summaries[later, 1] + summaries[later, 0] * carried
        carried = jnp.where(later > lax.axis_index("sp"), longer, carried)
    out_weight_grad = jnp.sum(products.astype(jnp.float32), axis=0)
    state_grad = local_sum + decay_prod * carried[:, None]
    grad_log = (
        state_grad * prior_vals * decay_val
        - state_grad * input_gate * conv_vals * decay_val * decay_val / norm_scale
    )
    grad_recur = (grad_log * -RATE_SCALE * softened * recur_gate * (1.0 - recur_gate)).astype(
        jnp.bfloat16
    )
    grad_input = (state_grad * norm_scale * conv_vals * input_gate * (1.0 - input_gate)).astype(
        jnp.bfloat16
    )
    back_recur = jnp.einsum(
        "hij,hjt->hit",
        w_recur,
        grad_recur.reshape(head_count, HEAD_DIM, length),
        preferred_element_type=jnp.float32,
    ).reshape(channels, length)
    back_input = jnp.einsum(
        "hij,hjt->hit",
        w_input,
        grad_input.reshape(head_count, HEAD_DIM, length),
        preferred_element_type=jnp.float32,
    ).reshape(channels, length)
    conv_grad = (state_grad * norm_scale * input_gate + back_recur + back_input).astype(
        jnp.bfloat16
    )
    return (gate_grad, up_grad, down_grad, out_weight_grad, conv_grad, valve_logit_derivative)


def solution(mesh):
    in_specs = (
        P("sp", "tp"),
        P("sp", "tp"),
        P("sp", None),
        P("sp", None),
        P("sp", None, "tp"),
        P("sp", None, "tp"),
        P("sp", "tp", None),
        P("tp", None),
        P("tp", "sp"),
        P("tp", "sp"),
        P("tp", "sp"),
        P(),
        P(),
        P(),
        P("tp", "sp"),
    )
    out_specs = (
        P("sp", None, "tp"),
        P("sp", None, "tp"),
        P("sp", "tp", None),
        P("tp", "sp"),
        P("tp", "sp"),
        P("tp", "sp"),
    )
    return jax.shard_map(local, mesh=mesh, in_specs=in_specs, out_specs=out_specs, check_vma=False)
```
